128 devices in a mesh: fs: 32 (over z, y, core), tp: 4 (over x).
Axes of the slice: x: 4, y: 4, z: 4, core: 2. Of those that a mesh axis runs over, the one named last changes fastest.
Arguments:
- model_input: bfloat16 [65536, 2048], P('fs'), may hold values from -6 to 6
- value_cotan: bfloat16 [65536, 2048], P('fs', 'tp'), may hold values from -0.0234375 to 0.0234375
- mixer_cotan: bfloat16 [65536, 2048], P('fs'), may hold values from -0.0234375 to 0.0234375
- head_output: bfloat16 [65536, 2048], P('fs', 'tp'), may hold values from -6 to 6
- value_weight: float32 [2048, 2048], P('fs', 'tp'), may hold values from -0.125 to 0.125
- value_factor: bfloat16 [2048, 512], P('fs'), may hold values from -0.125 to 0.125
- value_first: float32 [512, 2048], P('fs', 'tp'), may hold values from -3 to 3
- value_second: float32 [512, 2048], P('fs', 'tp'), may hold values from 0.02 to 0.5
- output_weight: float32 [2048, 2048], P('fs', 'tp'), may hold values from -0.125 to 0.125
- output_factor: bfloat16 [2048, 512], P('fs'), may hold values from -0.125 to 0.125
- output_first: float32 [512, 2048], P('fs', 'tp'), may hold values from -3 to 3
- output_second: float32 [512, 2048], P('fs', 'tp'), may hold values from 0.02 to 0.5
Outputs:
- value_step: float32 [2048, 2048], P('fs', 'tp')
- value_updated: float32 [2048, 2048], P('fs', 'tp')
- value_first_new: float32 [512, 2048], P('fs', 'tp')
- value_second_new: float32 [512, 2048], P('fs', 'tp')
- value_copy: bfloat16 [2048, 2048], P(None, 'tp')
- output_step: float32 [2048, 2048], P('fs', 'tp')
- output_updated: float32 [2048, 2048], P('fs', 'tp')
- output_first_new: float32 [512, 2048], P('fs', 'tp')
- output_second_new: float32 [512, 2048], P('fs', 'tp')
- output_copy: bfloat16 [2048, 2048], P(None, 'tp')
The draws below stay inside these ranges and needn't reach their ends.
All inputs are finite; a program needn't handle non-finite values.
Results may differ from the reference program's by a relative error of at most 0.0059.
Values may be sent and summed in bfloat16 or wider, within the bound.
No kernel may reach another device: no remote copies, remote signals or barrier semaphores. Data moves between devices by JAX's collectives and lax.ppermute only.
A program may use at most 128 MiB of HBM per device.

```python
import math
import jax
import jax.numpy as jnp
from jax import lax

D = 2048
RANK = 512
TOK_DEV = 2048
HV = 2048
TOKENS = 65536
N_FS = 32


def with_spikes(array, stream_key, source, target, blocks, factor):
    def block_of(dim):
        return (jnp.arange(array.shape[dim]) // (array.shape[dim] // blocks)).reshape((-1,) + (1,) * (array.ndim - 1 - dim))

    near = jax.random.permutation(stream_key, blocks)[block_of(target)]
    second = (block_of(target) + blocks // 2) % blocks
    return jnp.where((block_of(source) == near) | (block_of(source) == second), factor * array, array)


def steps_of(stream_key, extent, shards, low, high):
    level, own = 1.0, jax.random.fold_in(stream_key, 6)
    for position, shards_of in shards:
        steps = jnp.exp(jax.random.uniform(jax.random.fold_in(own, position), (shards_of,), jnp.float32, low / len(shards), high / len(shards)))
        level = level * jnp.repeat(steps, extent[position] // shards_of).reshape([-1 if axis == position else 1 for axis in range(len(extent))])
    return level


def bell_draw(own_key, extent, spread, limit, shards=(), dtype=jnp.bfloat16):
    array = jax.random.normal(own_key, extent, jnp.float32) * spread
    if len(shards) > 0:
        array = steps_of(own_key, extent, shards, -0.22, 0.18) * array
    return jnp.clip(array, min=-limit, max=limit).astype(dtype)


def noise_with(own_key, extent, spread, bound, cuts, heavy, kind=jnp.bfloat16):
    result = spread * jax.random.normal(own_key, extent, jnp.float32)
    if cuts:
        result = result * steps_of(own_key, extent, cuts, -0.22, 0.18)
    return jnp.clip(with_spikes(result, jax.random.fold_in(own_key, 3), *heavy), -bound, bound).astype(kind)


def setup_inputs(seed: int = 0) -> dict:
    arg_keys = jax.random.split(jax.random.key(seed), 13)
    model_input = noise_with(arg_keys[0], (TOKENS, D), 1.0, 6.0, ((0, 32),), (0, 1, 32, 2.75))
    value_cotan = bell_draw(arg_keys[1], (TOKENS, HV), ((TOK_DEV * N_FS) ** -0.5), 0.0234375, ((0, 32), (1, 4)))
    mixer_cotan = noise_with(arg_keys[2], (TOKENS, D), ((TOK_DEV * N_FS) ** -0.5), 0.0234375, ((0, 32),), (0, 1, 32, 2.75))
    head_output = bell_draw(arg_keys[3], (TOKENS, HV), 1.0, 6.0, ((0, 32), (1, 4)))
    value_weight = bell_draw(arg_keys[4], (D, HV), D ** -0.5, 0.125, ((0, 32), (1, 4)), jnp.float32)
    value_factor = bell_draw(arg_keys[5], (D, RANK), D ** -0.5, 0.125, ((0, 32),))
    value_first = bell_draw(arg_keys[6], (RANK, HV), 0.5, 3.0, ((0, 32), (1, 4)), jnp.float32)
    value_second = jnp.clip(jnp.exp(math.log(0.5) - 3.218876 * jax.random.uniform(arg_keys[7], (RANK, HV), jnp.float32) ** steps_of(arg_keys[7], (RANK, HV), ((0, 32), (1, 4)), -0.2, 0.2)), 0.02, 0.5)
    output_weight = bell_draw(arg_keys[8], (D, HV), HV ** -0.5, 0.125, ((0, 32), (1, 4)), jnp.float32)
    output_factor = bell_draw(arg_keys[9], (D, RANK), D ** -0.5, 0.125, ((0, 32),))
    output_first = bell_draw(arg_keys[10], (RANK, HV), 0.5, 3.0, ((0, 32), (1, 4)), jnp.float32)
    output_second = jnp.clip(jnp.exp(math.log(0.5) - 3.218876 * jax.random.uniform(arg_keys[11], (RANK, HV), jnp.float32) ** steps_of(arg_keys[11], (RANK, HV), ((0, 32), (1, 4)), -0.2, 0.2)), 0.02, 0.5)
    return dict(model_input=model_input, value_cotan=value_cotan, mixer_cotan=mixer_cotan, head_output=head_output, value_weight=value_weight, value_factor=value_factor, value_first=value_first, value_second=value_second, output_weight=output_weight, output_factor=output_factor, output_first=output_first, output_second=output_second)


beta_first = 0.8
beta_second = 0.9
step_rate = 0.02
scale_floor = 0.25
tiny_eps = 1e-08

def low_rank(rows_in, cols_in, factor, first_moment, second_moment):
    gradient = jnp.dot(rows_in.T, cols_in, preferred_element_type=jnp.float32)
    projected = jnp.dot(factor.astype(jnp.float32).T, gradient, precision=lax.Precision.HIGHEST)
    first_new = beta_first * first_moment + (1.0 - beta_first) * projected
    second_new = beta_second * second_moment + (1.0 - beta_second) * projected * projected
    direction = (first_new / (jnp.sqrt(second_new) + tiny_eps)).astype(jnp.bfloat16)
    expanded = jnp.dot(factor, direction, preferred_element_type=jnp.float32)
    return (expanded, first_new, second_new)

def finish(expanded, weight):
    mean_square = jnp.sum(expanded * expanded) / (D * HV)
    update_step = step_rate / jnp.sqrt(mean_square + scale_floor) * expanded
    updated = weight - update_step
    return (update_step, updated, updated.astype(jnp.bfloat16))

def reference(model_input, value_cotan, mixer_cotan, head_output, value_weight, value_factor, value_first, value_second, output_weight, output_factor, output_first, output_second):
    value_exp, value_fnew, value_snew = low_rank(model_input, value_cotan, value_factor, value_first, value_second)
    output_exp, output_fnew, output_snew = low_rank(mixer_cotan, head_output, output_factor, output_first, output_second)
    value_step, value_updated, value_copy = finish(value_exp, value_weight)
    output_step, output_updated, output_copy = finish(output_exp, output_weight)
    return (value_step, value_updated, value_fnew, value_snew, value_copy, output_step, output_updated, output_fnew, output_snew, output_copy)
```

```python
import jax
import jax.numpy as jnp
from jax import lax
from jax.sharding import Mesh
from jax.sharding import PartitionSpec as P

D = 2048
HV = 2048
ZY = ("fs_0", "fs_1")
CORE = "fs_2"
FS = ("fs_0", "fs_1", "fs_2")
N_ZY = 16

beta_first = 0.8
beta_second = 0.9
step_rate = 0.02
scale_floor = 0.25
tiny_eps = 1e-08


SWAP = [(0, 1), (1, 0)]


def swapped(x):
    return lax.ppermute(x, CORE, SWAP)


def sent_to_chips(x):
    copies = jnp.broadcast_to(x, (N_ZY, *x.shape))
    parts = lax.all_to_all(copies, ZY, split_axis=0, concat_axis=0, tiled=True)
    return parts.reshape(N_ZY * x.shape[0], x.shape[1])


def token_sum(rows_in, cols_in):
    return lax.dot_general(
        rows_in, cols_in, (((0,), (0,)), ((), ())), preferred_element_type=jnp.float32
    )


def local(
    model_input,
    value_cotan,
    mixer_cotan,
    head_output,
    value_weight,
    value_factor,
    value_first,
    value_second,
    output_weight,
    output_factor,
    output_first,
    output_second,
):
    core = lax.axis_index(CORE)
    first_core = core == 0
    fs_index = lax.axis_index(FS)

    def pick(a, b):
        return jnp.where(first_core, a, b)

    def chip_rows(mine, theirs):
        return pick(
            jnp.concatenate([mine, theirs], axis=0), jnp.concatenate([theirs, mine], axis=0)
        )

    factor_mine = pick(value_factor, output_factor)
    factor_theirs = swapped(pick(output_factor, value_factor))
    factor = sent_to_chips(chip_rows(factor_mine, factor_theirs))

    weights = jnp.concatenate([value_weight, output_weight], axis=1).astype(jnp.bfloat16)
    weights = lax.all_gather(weights, FS, axis=0, tiled=True)

    value_grad = token_sum(model_input, value_cotan)
    value_sent = lax.ppermute(value_grad.astype(jnp.bfloat16), CORE, [(1, 0)])
    output_grad = token_sum(mixer_cotan, head_output)
    output_sent = lax.ppermute(output_grad.astype(jnp.bfloat16), CORE, [(0, 1)])
    gradient = pick(
        value_grad + value_sent.astype(jnp.float32), output_grad + output_sent.astype(jnp.float32)
    ).astype(jnp.bfloat16)

    moments_mine = jnp.concatenate(
        [pick(value_first, output_first), pick(value_second, output_second)], axis=1
    )
    moments_theirs = swapped(
        jnp.concatenate(
            [pick(output_first, value_first), pick(output_second, value_second)], axis=1
        )
    )
    moments = chip_rows(moments_mine, moments_theirs)

    part = token_sum(factor, gradient).astype(jnp.bfloat16)
    parts = lax.all_to_all(
        part.reshape(N_ZY, 32, 512), ZY, split_axis=0, concat_axis=0, tiled=True
    )
    projected = parts.astype(jnp.float32).sum(axis=0)
    first_new = beta_first * moments[:, :512] + (1.0 - beta_first) * projected
    second_new = beta_second * moments[:, 512:] + (1.0 - beta_second) * projected * projected
    direction = (first_new / (jnp.sqrt(second_new) + tiny_eps)).astype(jnp.bfloat16)
    direction = sent_to_chips(direction)

    gram = token_sum(factor, factor)
    gram_high = lax.optimization_barrier(gram.astype(jnp.bfloat16))
    gram_low = (gram - gram_high.astype(jnp.float32)).astype(jnp.bfloat16)
    turned = jnp.dot(gram_high, direction, preferred_element_type=jnp.float32) + jnp.dot(
        gram_low, direction, preferred_element_type=jnp.float32
    )
    square = jnp.sum(turned * direction.astype(jnp.float32)).reshape(1, 1)
    others = [
        lax.ppermute(square, "tp", [(i, (i + k) % 4) for i in range(4)]) for k in (1, 2, 3)
    ]
    square = square + others[0] + others[1] + others[2]
    square_theirs = swapped(square)
    value_sq, output_sq = pick(square, square_theirs), pick(square_theirs, square)

    factor_theirs = swapped(factor)
    direction_theirs = swapped(direction)
    value_exp = jnp.dot(
        pick(factor, factor_theirs),
        pick(direction, direction_theirs),
        preferred_element_type=jnp.float32,
    )
    output_exp = jnp.dot(
        pick(factor_theirs, factor),
        pick(direction_theirs, direction),
        preferred_element_type=jnp.float32,
    )
    value_scale = step_rate / jnp.sqrt(value_sq / (D * HV) + scale_floor)
    output_scale = step_rate / jnp.sqrt(output_sq / (D * HV) + scale_floor)
    value_copy = (weights[:, :512].astype(jnp.float32) - value_scale * value_exp).astype(
        jnp.bfloat16
    )
    output_copy = (weights[:, 512:].astype(jnp.float32) - output_scale * output_exp).astype(
        jnp.bfloat16
    )
    value_step = value_scale * lax.dynamic_slice_in_dim(value_exp, fs_index * 64, 64, 0)
    output_step = output_scale * lax.dynamic_slice_in_dim(output_exp, fs_index * 64, 64, 0)
    value_updated = value_weight - value_step
    output_updated = output_weight - output_step

    news = jnp.concatenate([first_new, second_new], axis=1)
    upper, lower = news[:16], news[16:]
    news_mine = pick(upper, lower)
    news_theirs = swapped(pick(lower, upper))
    value_news, output_news = pick(news_mine, news_theirs), pick(news_theirs, news_mine)
    return (
        value_step,
        value_updated,
        value_news[:, :512],
        value_news[:, 512:],
        value_copy,
        output_step,
        output_updated,
        output_news[:, :512],
        output_news[:, 512:],
        output_copy,
    )


def solution(mesh):
    torus = Mesh(mesh.devices.reshape(4, 4, 2, mesh.shape["tp"]), ("fs_0", "fs_1", "fs_2", "tp"))
    in_specs = (
        P(FS, None),
        P(FS, "tp"),
        P(FS, None),
        P(FS, "tp"),
        P(FS, "tp"),
        P(FS, None),
        P(FS, "tp"),
        P(FS, "tp"),
        P(FS, "tp"),
        P(FS, None),
        P(FS, "tp"),
        P(FS, "tp"),
    )
    out_specs = (
        P(FS, "tp"),
        P(FS, "tp"),
        P(FS, "tp"),
        P(FS, "tp"),
        P(None, "tp"),
        P(FS, "tp"),
        P(FS, "tp"),
        P(FS, "tp"),
        P(FS, "tp"),
        P(None, "tp"),
    )
    return jax.shard_map(local, mesh=torus, in_specs=in_specs, out_specs=out_specs, check_vma=False)
```

```python
import jax
import jax.numpy as jnp
from jax import lax
from jax.sharding import Mesh
from jax.sharding import PartitionSpec as P
from jax.experimental import pallas as pl
from jax.experimental.pallas import tpu as pltpu

D = 2048
HV = 2048
ZY = ("fs_0", "fs_1")
CORE = "fs_2"
FS = ("fs_0", "fs_1", "fs_2")
N_ZY = 16

beta_first = 0.8
beta_second = 0.9
step_rate = 0.02
scale_floor = 0.25
tiny_eps = 1e-08

SWAP = [(0, 1), (1, 0)]


def swapped(x):
    return lax.ppermute(x, CORE, SWAP)


def sent_to_chips(x):
    copies = jnp.broadcast_to(x, (N_ZY, *x.shape))
    parts = lax.all_to_all(copies, ZY, split_axis=0, concat_axis=0, tiled=True)
    return parts.reshape(N_ZY * x.shape[0], x.shape[1])


def place(z, y, core):
    return (z % 4 * 4 + y % 4) * 2 + core


def ring_pairs(shift, along_y_core):
    pairs = []
    for z in range(4):
        for y in range(4):
            for core in range(2):
                to = (z, y - shift) if core == along_y_core else (z - shift, y)
                pairs.append((place(z, y, core), place(*to, core)))
    return pairs


def order_kernel(index_ref, *refs):
    out_ref = refs[-1]
    for b in range(4):
        for a in range(4):
            out_ref[index_ref[b * 4 + a]] = refs[b][a]


def in_chip_order(groups, index):
    vmem = pl.BlockSpec(memory_space=pltpu.VMEM)
    return pl.pallas_call(
        order_kernel,
        in_specs=[pl.BlockSpec(memory_space=pltpu.SMEM)] + [vmem] * 4,
        out_specs=vmem,
        out_shape=jax.ShapeDtypeStruct((N_ZY, 128, 512), jnp.bfloat16),
        compiler_params=pltpu.CompilerParams(vmem_limit_bytes=8 << 20),
        name="in_chip_order",
    )(index, *groups)


def gradient_kernel(core_ref, rows0, rows1, cols0, cols1, out_ref, rows_buf, cols_buf, turned, row_sems, col_sem):
    step=pl.program_id(0); steps=pl.num_programs(0); slot=step%2
    wide=out_ref.shape[1]
    def rows_copy(rows, at, half):
        return pltpu.make_async_copy(rows.at[:, pl.ds(at*wide,wide)], rows_buf.at[half], row_sems.at[half])
    def cols_copy(cols):
        return pltpu.make_async_copy(cols, cols_buf, col_sem)
    def fetch(at, half):
        @pl.when(core_ref[0]==0)
        def _():
            rows_copy(rows0,at,half).start()
        @pl.when(core_ref[0]!=0)
        def _():
            rows_copy(rows1,at,half).start()
    @pl.when(step==0)
    def _():
        @pl.when(core_ref[0]==0)
        def _():
            cols_copy(cols0).start()
        @pl.when(core_ref[0]!=0)
        def _():
            cols_copy(cols1).start()
        fetch(0,0)
    @pl.when(step+1<steps)
    def _():
        fetch(step+1,1-slot)
    @pl.when(step==0)
    def _():
        cols_copy(cols0).wait()
        turned[...]=cols_buf[...].T
    rows_copy(rows0,step,slot).wait()
    out_ref[...]=jnp.dot(turned[...],rows_buf[slot],preferred_element_type=jnp.float32).astype(jnp.bfloat16)


def gradient(core, rows0, rows1, cols0, cols1, wide=512):
    hbm=pl.BlockSpec(memory_space=pltpu.HBM)
    return pl.pallas_call(gradient_kernel, grid=(2048//wide,),
      in_specs=[pl.BlockSpec(memory_space=pltpu.SMEM)]+[hbm]*4,
      out_specs=pl.BlockSpec((512,wide),lambda i:(0,i)),
      out_shape=jax.ShapeDtypeStruct((512,2048),jnp.bfloat16),
      scratch_shapes=[pltpu.VMEM((2,2048,wide),jnp.bfloat16),pltpu.VMEM((2048,512),jnp.bfloat16),pltpu.VMEM((512,2048),jnp.bfloat16),pltpu.SemaphoreType.DMA((2,)),pltpu.SemaphoreType.DMA],
      compiler_params=pltpu.CompilerParams(vmem_limit_bytes=57 << 20), name="gradient")(core, rows0, rows1, cols0, cols1)


CHUNKS = 8


def finish_kernel(
    core_ref,
    square,
    f0,
    f1,
    d0,
    d1,
    w0,
    w1,
    value_exp,
    output_exp,
    value_weight,
    output_weight,
    value_copy,
    output_copy,
    value_step,
    value_updated,
    output_step,
    output_updated,
    tiles,
    sems,
):
    rows = D // CHUNKS
    first_core = core_ref[0] == 0

    def scale_of(sums):
        return step_rate / jnp.sqrt(jnp.sum(sums, keepdims=True) / (D * HV) + scale_floor)

    value_scale = scale_of(square[:4].sum(axis=0))
    output_scale = scale_of(square[4:].sum(axis=0))
    scales = (
        jnp.where(first_core, value_scale, output_scale),
        jnp.where(first_core, output_scale, value_scale),
    )

    def sent(out, which, chunk):
        at = pl.ds(chunk * rows, rows)
        return pltpu.make_async_copy(tiles.at[which, at], out.at[at], sems.at[which, chunk])

    for chunk in range(CHUNKS):
        at = pl.ds(chunk * rows, rows)
        for which, (f, d, w) in enumerate(((f0, d0, w0), (f1, d1, w1))):
            whole = jnp.dot(f[at], d[...], preferred_element_type=jnp.float32)
            tile = w[at].astype(jnp.float32) - scales[which] * whole
            tiles[which, at] = tile.astype(jnp.bfloat16)

        @pl.when(first_core)
        def _():
            sent(value_copy, 0, chunk).start()
            sent(output_copy, 1, chunk).start()

        @pl.when(jnp.logical_not(first_core))
        def _():
            sent(output_copy, 0, chunk).start()
            sent(value_copy, 1, chunk).start()

    for scale, exp, weight, step, updated in (
        (value_scale, value_exp, value_weight, value_step, value_updated),
        (output_scale, output_exp, output_weight, output_step, output_updated),
    ):
        step[...] = scale * exp[...]
        updated[...] = weight[...] - scale * exp[...]

    for chunk in range(CHUNKS):
        for which in (0, 1):
            sent(value_copy, which, chunk).wait()


def finish(core, *arrays):
    smem = pl.BlockSpec(memory_space=pltpu.SMEM)
    vmem = pl.BlockSpec(memory_space=pltpu.VMEM)
    hbm = pl.BlockSpec(memory_space=pltpu.HBM)
    copy = jax.ShapeDtypeStruct((D, 512), jnp.bfloat16)
    local = jax.ShapeDtypeStruct((64, 512), jnp.float32)
    return pl.pallas_call(
        finish_kernel,
        in_specs=[smem] + [vmem] * 11,
        out_specs=[hbm] * 2 + [vmem] * 4,
        out_shape=[copy] * 2 + [local] * 4,
        scratch_shapes=[
            pltpu.VMEM((2, D, 512), jnp.bfloat16),
            pltpu.SemaphoreType.DMA((2, CHUNKS)),
        ],
        compiler_params=pltpu.CompilerParams(vmem_limit_bytes=12 << 20),
        name="finish",
    )(core, *arrays)


def token_sum(rows_in, cols_in):
    return lax.dot_general(
        rows_in, cols_in, (((0,), (0,)), ((), ())), preferred_element_type=jnp.float32
    )


def local(
    model_input,
    value_cotan,
    mixer_cotan,
    head_output,
    value_weight,
    value_factor,
    value_first,
    value_second,
    output_weight,
    output_factor,
    output_first,
    output_second,
):
    core = lax.axis_index(CORE)
    first_core = core == 0

    def pick(a, b):
        return jnp.where(first_core, a, b)

    def chip_rows(mine, theirs):
        return pick(
            jnp.concatenate([mine, theirs], axis=0), jnp.concatenate([theirs, mine], axis=0)
        )

    factor_theirs = swapped(pick(output_factor, value_factor))
    rows = chip_rows(pick(value_factor, output_factor), factor_theirs)
    group = [rows] + [lax.ppermute(rows, FS, ring_pairs(k, 0)) for k in (1, 2, 3)]
    group = jnp.stack(group)
    weights = lax.optimization_barrier((value_weight, output_weight, group[:1, :8, :128]))[:2]
    value_rows, output_rows = (w.astype(jnp.bfloat16) for w in weights)
    weight_rows = chip_rows(pick(value_rows, output_rows), swapped(pick(output_rows, value_rows)))
    weight = lax.all_gather(weight_rows, ZY, axis=0, tiled=True)
    groups = [group] + [lax.ppermute(group, FS, ring_pairs(k, 1)) for k in (1, 2, 3)]
    z, y = lax.axis_index("fs_0"), lax.axis_index("fs_1")
    step_b, step_a = jnp.arange(16) // 4, jnp.arange(16) % 4
    index = pick((z + step_b) % 4 * 4 + (y + step_a) % 4, (z + step_a) % 4 * 4 + (y + step_b) % 4)
    factor = in_chip_order(groups, index.astype(jnp.int32)).reshape(2048, 512)

    arrays = (model_input, mixer_cotan, value_cotan, head_output)
    grad_theirs = gradient(1 - core.reshape(1), *arrays)
    grad_sent = swapped(grad_theirs)
    grad_mine = gradient(core.reshape(1), *arrays)
    grad_sum = (grad_mine.astype(jnp.float32) + grad_sent.astype(jnp.float32)).astype(jnp.bfloat16)
    grad_sum = lax.optimization_barrier(grad_sum)

    moments_mine = jnp.concatenate(
        [pick(value_first, output_first), pick(value_second, output_second)], axis=1
    )
    moments_theirs = swapped(
        jnp.concatenate(
            [pick(output_first, value_first), pick(output_second, value_second)], axis=1
        )
    )
    moments = chip_rows(moments_mine, moments_theirs)

    part = lax.dot_general(
        factor, grad_sum, (((0,), (1,)), ((), ())), preferred_element_type=jnp.float32
    ).astype(jnp.bfloat16)
    parts = lax.all_to_all(part.reshape(N_ZY, 32, 512), ZY, split_axis=0, concat_axis=0, tiled=True)
    projected = parts.astype(jnp.float32).sum(axis=0)
    first_new = beta_first * moments[:, :512] + (1.0 - beta_first) * projected
    second_new = beta_second * moments[:, 512:] + (1.0 - beta_second) * projected * projected
    direction = (first_new / (jnp.sqrt(second_new) + tiny_eps)).astype(jnp.bfloat16)
    direction = sent_to_chips(direction)

    gram = token_sum(factor, factor)
    gram_high = lax.optimization_barrier(gram.astype(jnp.bfloat16))
    gram_low = (gram - gram_high.astype(jnp.float32)).astype(jnp.bfloat16)
    gram_low = lax.optimization_barrier(gram_low)
    turned = jnp.dot(gram_high, direction, preferred_element_type=jnp.float32) + jnp.dot(
        gram_low, direction, preferred_element_type=jnp.float32
    )
    square = (turned * direction.astype(jnp.float32)).reshape(64, 8, 4, 128)
    square = square.sum(axis=(0, 2))
    square = jnp.broadcast_to(square, (8, 8, 128))
    square = lax.all_to_all(square, (CORE, "tp"), split_axis=0, concat_axis=0, tiled=True)
    factor_other = swapped(factor)
    weight_other = swapped(weight)
    direction_other = swapped(direction)
    value_d, output_d = lax.optimization_barrier(
        (pick(direction, direction_other), pick(direction_other, direction))
    )
    value_exp = jnp.dot(value_factor, value_d, preferred_element_type=jnp.float32)
    output_exp = jnp.dot(output_factor, output_d, preferred_element_type=jnp.float32)
    value_exp, output_exp = lax.optimization_barrier((value_exp, output_exp))
    value_copy, output_copy, value_step, value_updated, output_step, output_updated = finish(
        core.reshape(1),
        square,
        factor,
        factor_other,
        direction,
        direction_other,
        weight,
        weight_other,
        value_exp,
        output_exp,
        value_weight,
        output_weight,
    )

    news = jnp.concatenate([first_new, second_new], axis=1)
    upper, lower = news[:16], news[16:]
    news_mine = pick(upper, lower)
    news_theirs = swapped(pick(lower, upper))
    value_news, output_news = pick(news_mine, news_theirs), pick(news_theirs, news_mine)
    return (
        value_step,
        value_updated,
        value_news[:, :512],
        value_news[:, 512:],
        value_copy,
        output_step,
        output_updated,
        output_news[:, :512],
        output_news[:, 512:],
        output_copy,
    )


def solution(mesh):
    torus = Mesh(mesh.devices.reshape(4, 4, 2, mesh.shape["tp"]), ("fs_0", "fs_1", "fs_2", "tp"))
    in_specs = (
        P(FS, None),
        P(FS, "tp"),
        P(FS, None),
        P(FS, "tp"),
        P(FS, "tp"),
        P(FS, None),
        P(FS, "tp"),
        P(FS, "tp"),
        P(FS, "tp"),
        P(FS, None),
        P(FS, "tp"),
        P(FS, "tp"),
    )
    out_specs = (
        P(FS, "tp"),
        P(FS, "tp"),
        P(FS, "tp"),
        P(FS, "tp"),
        P(None, "tp"),
        P(FS, "tp"),
        P(FS, "tp"),
        P(FS, "tp"),
        P(FS, "tp"),
        P(None, "tp"),
    )

    return jax.shard_map(local, mesh=torus, in_specs=in_specs, out_specs=out_specs, check_vma=False)
```

```python
import jax
import jax.numpy as jnp
from jax import lax
from jax.sharding import Mesh
from jax.sharding import PartitionSpec as P
from jax.experimental import pallas as pl
from jax.experimental.pallas import tpu as pltpu

D = 2048
HV = 2048
ZY = ("fs_0", "fs_1")
CORE = "fs_2"
FS = ("fs_0", "fs_1", "fs_2")
N_ZY = 16

beta_first = 0.8
beta_second = 0.9
step_rate = 0.02
scale_floor = 0.25
tiny_eps = 1e-08

SWAP = [(0, 1), (1, 0)]


def swapped(x):
    return lax.ppermute(x, CORE, SWAP)


def sent_to_chips(x):
    copies = jnp.broadcast_to(x, (N_ZY, *x.shape))
    parts = lax.all_to_all(copies, ZY, split_axis=0, concat_axis=0, tiled=True)
    return parts.reshape(N_ZY * x.shape[0], x.shape[1])


def place(z, y, core):
    return (z % 4 * 4 + y % 4) * 2 + core


def ring_pairs(shift, along_y_core):
    pairs = []
    for z in range(4):
        for y in range(4):
            for core in range(2):
                to = (z, y - shift) if core == along_y_core else (z - shift, y)
                pairs.append((place(z, y, core), place(*to, core)))
    return pairs


def order_kernel(index_ref, *refs):
    out_ref = refs[-1]
    for b in range(4):
        for a in range(4):
            out_ref[index_ref[b * 4 + a]] = refs[b][a]


def in_chip_order(groups, index):
    vmem = pl.BlockSpec(memory_space=pltpu.VMEM)
    return pl.pallas_call(
        order_kernel,
        in_specs=[pl.BlockSpec(memory_space=pltpu.SMEM)] + [vmem] * 4,
        out_specs=vmem,
        out_shape=jax.ShapeDtypeStruct((N_ZY, 128, 512), jnp.bfloat16),
        compiler_params=pltpu.CompilerParams(vmem_limit_bytes=8 << 20),
        name="in_chip_order",
    )(index, *groups)


BLOCKS = 2


def gradient_kernel(core_ref, *refs):
    rows, cols = refs[:2], refs[2:4]
    sent = refs[4:-6]
    out_ref, rows_buf, cols_buf, turned, rows_sems, cols_sems = refs[-6:]
    step = pl.program_id(0)
    wide = D // BLOCKS

    def rows_copy(which, block):
        at = pl.ds(block * wide, wide)
        return pltpu.make_async_copy(
            rows[which].at[:, at], rows_buf.at[block], rows_sems.at[block]
        )

    def cols_copy(which, block):
        at = pl.ds(block * wide, wide)
        return pltpu.make_async_copy(cols[which].at[at], cols_buf.at[at], cols_sems.at[block])

    @pl.when(step == 0)
    def _():
        for which in (0, 1):

            @pl.when(core_ref[0] == which)
            def _():
                for block in range(BLOCKS):
                    cols_copy(which, block).start()
                for block in range(BLOCKS):
                    rows_copy(which, block).start()

        for block in range(BLOCKS):
            cols_copy(0, block).wait()
            at = pl.ds(block * wide, wide)
            turned[:, at] = cols_buf[at].T

    rows_copy(0, step).wait()
    grad = jnp.dot(turned[...], rows_buf[step], preferred_element_type=jnp.float32)
    for ref in sent:
        grad = grad + ref[...].astype(jnp.float32)
    out_ref[...] = grad.astype(jnp.bfloat16)


def gradient(core, arrays, sent=()):
    hbm = pl.BlockSpec(memory_space=pltpu.HBM)
    wide = D // BLOCKS
    block = pl.BlockSpec((512, wide), lambda i: (0, i))
    return pl.pallas_call(
        gradient_kernel,
        grid=(BLOCKS,),
        in_specs=[pl.BlockSpec(memory_space=pltpu.SMEM)] + [hbm] * 4 + [block] * len(sent),
        out_specs=block,
        out_shape=jax.ShapeDtypeStruct((512, D), jnp.bfloat16),
        scratch_shapes=[
            pltpu.VMEM((BLOCKS, 2048, wide), jnp.bfloat16),
            pltpu.VMEM((2048, 512), jnp.bfloat16),
            pltpu.VMEM((512, 2048), jnp.bfloat16),
            pltpu.SemaphoreType.DMA((BLOCKS,)),
            pltpu.SemaphoreType.DMA((BLOCKS,)),
        ],
        compiler_params=pltpu.CompilerParams(vmem_limit_bytes=57 << 20),
        name="gradient",
    )(core, *arrays, *sent)


def square_kernel(high, low, direction, out_ref):
    d = direction[...]
    turned = jnp.dot(high[...], d, preferred_element_type=jnp.float32)
    turned = turned + jnp.dot(low[...], d, preferred_element_type=jnp.float32)
    sums = (turned * d.astype(jnp.float32)).reshape(64, 8, 512).sum(axis=0)
    sums = sums[:, :128] + sums[:, 128:256] + sums[:, 256:384] + sums[:, 384:]
    for i in range(8):
        out_ref[i] = sums


def square_sums(high, low, direction):
    vmem = pl.BlockSpec(memory_space=pltpu.VMEM)
    return pl.pallas_call(
        square_kernel,
        in_specs=[vmem] * 3,
        out_specs=vmem,
        out_shape=jax.ShapeDtypeStruct((8, 8, 128), jnp.float32),
        compiler_params=pltpu.CompilerParams(vmem_limit_bytes=8 << 20),
        name="square_sums",
    )(high, low, direction)


CHUNKS = 8


def finish_kernel(
    core_ref,
    at_ref,
    square,
    f0,
    f1,
    d0,
    d1,
    w0,
    w1,
    value_weight,
    output_weight,
    value_copy,
    output_copy,
    value_step,
    value_updated,
    output_step,
    output_updated,
    tiles,
    sems,
):
    rows = D // CHUNKS
    first_core = core_ref[0] == 0

    def scale_of(sums):
        return step_rate / jnp.sqrt(jnp.sum(sums, keepdims=True) / (D * HV) + scale_floor)

    value_scale = scale_of(square[:4].sum(axis=0))
    output_scale = scale_of(square[4:].sum(axis=0))
    scales = (
        jnp.where(first_core, value_scale, output_scale),
        jnp.where(first_core, output_scale, value_scale),
    )

    def sent(out, which, chunk):
        at = pl.ds(chunk * rows, rows)
        return pltpu.make_async_copy(tiles.at[which, at], out.at[at], sems.at[which, chunk])

    for chunk in range(CHUNKS):
        at = pl.ds(chunk * rows, rows)
        for which, (f, d, w) in enumerate(((f0, d0, w0), (f1, d1, w1))):
            whole = jnp.dot(f[at], d[...], preferred_element_type=jnp.float32)
            tile = w[at].astype(jnp.float32) - scales[which] * whole
            tiles[which, at] = tile.astype(jnp.bfloat16)

        @pl.when(first_core)
        def _():
            sent(value_copy, 0, chunk).start()
            sent(output_copy, 1, chunk).start()

        @pl.when(jnp.logical_not(first_core))
        def _():
            sent(output_copy, 0, chunk).start()
            sent(value_copy, 1, chunk).start()

    local = pl.ds(pl.multiple_of(at_ref[0], 64), 64)
    steps = [
        scale * jnp.dot(f[local], d[...], preferred_element_type=jnp.float32)
        for scale, f, d in zip(scales, (f0, f1), (d0, d1))
    ]

    @pl.when(first_core)
    def _():
        value_step[...], output_step[...] = steps

    @pl.when(jnp.logical_not(first_core))
    def _():
        output_step[...], value_step[...] = steps

    value_updated[...] = value_weight[...] - value_step[...]
    output_updated[...] = output_weight[...] - output_step[...]

    for chunk in range(CHUNKS):
        for which in (0, 1):
            sent(value_copy, which, chunk).wait()


def finish(core, at, *arrays):
    smem = pl.BlockSpec(memory_space=pltpu.SMEM)
    vmem = pl.BlockSpec(memory_space=pltpu.VMEM)
    hbm = pl.BlockSpec(memory_space=pltpu.HBM)
    copy = jax.ShapeDtypeStruct((D, 512), jnp.bfloat16)
    local = jax.ShapeDtypeStruct((64, 512), jnp.float32)
    return pl.pallas_call(
        finish_kernel,
        in_specs=[smem] * 2 + [vmem] * 9,
        out_specs=[hbm] * 2 + [vmem] * 4,
        out_shape=[copy] * 2 + [local] * 4,
        scratch_shapes=[
            pltpu.VMEM((2, D, 512), jnp.bfloat16),
            pltpu.SemaphoreType.DMA((2, CHUNKS)),
        ],
        compiler_params=pltpu.CompilerParams(vmem_limit_bytes=12 << 20),
        name="finish",
    )(core, at, *arrays)


def token_sum(rows_in, cols_in):
    return lax.dot_general(
        rows_in, cols_in, (((0,), (0,)), ((), ())), preferred_element_type=jnp.float32
    )


def local(
    model_input,
    value_cotan,
    mixer_cotan,
    head_output,
    value_weight,
    value_factor,
    value_first,
    value_second,
    output_weight,
    output_factor,
    output_first,
    output_second,
):
    core = lax.axis_index(CORE)
    first_core = core == 0

    def pick(a, b):
        return jnp.where(first_core, a, b)

    def chip_rows(mine, theirs):
        return pick(
            jnp.concatenate([mine, theirs], axis=0), jnp.concatenate([theirs, mine], axis=0)
        )

    value_rows = jnp.concatenate([value_factor, value_weight.astype(jnp.bfloat16)], axis=1)
    output_rows = jnp.concatenate([output_factor, output_weight.astype(jnp.bfloat16)], axis=1)
    rows = chip_rows(
        pick(value_rows, output_rows), swapped(pick(output_rows, value_rows))
    )
    group = [rows] + [lax.ppermute(rows, FS, ring_pairs(k, 0)) for k in (1, 2, 3)]
    group, weight_group = lax.optimization_barrier(
        (jnp.stack([g[:, :512] for g in group]), jnp.stack([g[:, 512:] for g in group]))
    )
    groups = [group] + [lax.ppermute(group, FS, ring_pairs(k, 1)) for k in (1, 2, 3)]
    weight_groups = [weight_group] + [
        lax.ppermute(weight_group, FS, ring_pairs(k, 1)) for k in (1, 2, 3)
    ]
    z, y = lax.axis_index("fs_0"), lax.axis_index("fs_1")
    step_b, step_a = jnp.arange(16) // 4, jnp.arange(16) % 4
    index = pick((z + step_b) % 4 * 4 + (y + step_a) % 4, (z + step_a) % 4 * 4 + (y + step_b) % 4)
    index = index.astype(jnp.int32)
    factor = in_chip_order(groups, index).reshape(2048, 512)

    arrays = (model_input, mixer_cotan, value_cotan, head_output)
    grad_theirs = gradient(1 - core.reshape(1), arrays)
    grad_sent = swapped(grad_theirs)
    grad_sum = gradient(core.reshape(1), arrays, (grad_sent,))

    moments_mine = jnp.concatenate(
        [pick(value_first, output_first), pick(value_second, output_second)], axis=1
    )
    moments_theirs = swapped(
        jnp.concatenate(
            [pick(output_first, value_first), pick(output_second, value_second)], axis=1
        )
    )
    moments = chip_rows(moments_mine, moments_theirs)

    part = lax.dot_general(
        factor, grad_sum, (((0,), (1,)), ((), ())), preferred_element_type=jnp.float32
    ).astype(jnp.bfloat16)
    parts = lax.all_to_all(part.reshape(N_ZY, 32, 512), ZY, split_axis=0, concat_axis=0, tiled=True)
    projected = parts.astype(jnp.float32).sum(axis=0)
    first_new = beta_first * moments[:, :512] + (1.0 - beta_first) * projected
    second_new = beta_second * moments[:, 512:] + (1.0 - beta_second) * projected * projected
    direction = (first_new / (jnp.sqrt(second_new) + tiny_eps)).astype(jnp.bfloat16)
    direction = sent_to_chips(direction)

    gram = token_sum(factor, factor)
    gram_high = lax.optimization_barrier(gram.astype(jnp.bfloat16))
    gram_low = (gram - gram_high.astype(jnp.float32)).astype(jnp.bfloat16)
    gram_low = lax.optimization_barrier(gram_low)
    square = square_sums(gram_high, gram_low, direction)
    square = lax.all_to_all(square, (CORE, "tp"), split_axis=0, concat_axis=0, tiled=True)
    factor_other = swapped(factor)
    weight = in_chip_order(weight_groups, index).reshape(2048, 512)
    weight_other = swapped(weight)
    direction_other = swapped(direction)
    value_copy, output_copy, value_step, value_updated, output_step, output_updated = finish(
        core.reshape(1),
        (lax.axis_index(FS) * 64).reshape(1),
        square,
        factor,
        factor_other,
        direction,
        direction_other,
        weight,
        weight_other,
        value_weight,
        output_weight,
    )

    news = jnp.concatenate([first_new, second_new], axis=1)
    upper, lower = news[:16], news[16:]
    news_mine = pick(upper, lower)
    news_theirs = swapped(pick(lower, upper))
    value_news, output_news = pick(news_mine, news_theirs), pick(news_theirs, news_mine)
    value_fnew, value_snew = value_news[:, :512], value_news[:, 512:]
    output_fnew, output_snew = output_news[:, :512], output_news[:, 512:]
    return (
        value_step,
        value_updated,
        value_fnew,
        value_snew,
        value_copy,
        output_step,
        output_updated,
        output_fnew,
        output_snew,
        output_copy,
    )


def solution(mesh):
    torus = Mesh(mesh.devices.reshape(4, 4, 2, mesh.shape["tp"]), ("fs_0", "fs_1", "fs_2", "tp"))
    in_specs = (
        P(FS, None),
        P(FS, "tp"),
        P(FS, None),
        P(FS, "tp"),
        P(FS, "tp"),
        P(FS, None),
        P(FS, "tp"),
        P(FS, "tp"),
        P(FS, "tp"),
        P(FS, None),
        P(FS, "tp"),
        P(FS, "tp"),
    )
    out_specs = (
        P(FS, "tp"),
        P(FS, "tp"),
        P(FS, "tp"),
        P(FS, "tp"),
        P(None, "tp"),
        P(FS, "tp"),
        P(FS, "tp"),
        P(FS, "tp"),
        P(FS, "tp"),
        P(None, "tp"),
    )

    return jax.shard_map(local, mesh=torus, in_specs=in_specs, out_specs=out_specs, check_vma=False)
```

```python
import jax
import jax.numpy as jnp
from jax import lax
from jax.sharding import Mesh
from jax.sharding import PartitionSpec as P
from jax.experimental import pallas as pl
from jax.experimental.pallas import tpu as pltpu

D = 2048
HV = 2048
ZY = ("fs_0", "fs_1")
CORE = "fs_2"
FS = ("fs_0", "fs_1", "fs_2")
N_ZY = 16

beta_first = 0.8
beta_second = 0.9
step_rate = 0.02
scale_floor = 0.25
tiny_eps = 1e-08

SWAP = [(0, 1), (1, 0)]


def swapped(x):
    return lax.ppermute(x, CORE, SWAP)


def sent_to_chips(x):
    copies = jnp.broadcast_to(x, (N_ZY, *x.shape))
    parts = lax.all_to_all(copies, ZY, split_axis=0, concat_axis=0, tiled=True)
    return parts.reshape(N_ZY * x.shape[0], x.shape[1])


def place(z, y, core):
    return (z % 4 * 4 + y % 4) * 2 + core


def ring_pairs(shift, along_y_core):
    pairs = []
    for z in range(4):
        for y in range(4):
            for core in range(2):
                to = (z, y - shift) if core == along_y_core else (z - shift, y)
                pairs.append((place(z, y, core), place(*to, core)))
    return pairs


def from_ring(x, along_y_core):
    received = []
    for shift in (1, 2, 3):
        received.append(lax.ppermute(x, FS, ring_pairs(shift, along_y_core)))
    return [x] + received


def order_kernel(index_ref, *refs):
    out_ref = refs[-1]
    for b in range(4):
        for a in range(4):
            out_ref[index_ref[b * 4 + a]] = refs[b][a]


def in_chip_order(groups, index):
    vmem = pl.BlockSpec(memory_space=pltpu.VMEM)
    return pl.pallas_call(
        order_kernel,
        in_specs=[pl.BlockSpec(memory_space=pltpu.SMEM)] + [vmem] * 4,
        out_specs=vmem,
        out_shape=jax.ShapeDtypeStruct((N_ZY, 128, 512), jnp.bfloat16),
        compiler_params=pltpu.CompilerParams(vmem_limit_bytes=8 << 20),
        name="in_chip_order",
    )(index, *groups)


BLOCKS = 2


def gradient_kernel(core_ref, *refs):
    rows, cols = refs[:2], refs[2:4]
    sent = refs[4:-6]
    out_ref, rows_buf, cols_buf, turned, rows_sems, cols_sems = refs[-6:]
    step = pl.program_id(0)
    wide = D // BLOCKS

    def rows_copy(which, block):
        at = pl.ds(block * wide, wide)
        return pltpu.make_async_copy(
            rows[which].at[:, at], rows_buf.at[block], rows_sems.at[block]
        )

    def cols_copy(which, block):
        at = pl.ds(block * wide, wide)
        return pltpu.make_async_copy(cols[which].at[at], cols_buf.at[at], cols_sems.at[block])

    @pl.when(step == 0)
    def _():
        for which in (0, 1):

            @pl.when(core_ref[0] == which)
            def _():
                for block in range(BLOCKS):
                    cols_copy(which, block).start()
                for block in range(BLOCKS):
                    rows_copy(which, block).start()

        for block in range(BLOCKS):
            cols_copy(0, block).wait()
            at = pl.ds(block * wide, wide)
            turned[:, at] = cols_buf[at].T

    rows_copy(0, step).wait()
    grad = jnp.dot(turned[...], rows_buf[step], preferred_element_type=jnp.float32)
    for ref in sent:
        grad = grad + ref[...].astype(jnp.float32)
    out_ref[...] = grad.astype(jnp.bfloat16)


def gradient(core, arrays, sent=()):
    hbm = pl.BlockSpec(memory_space=pltpu.HBM)
    wide = D // BLOCKS
    block = pl.BlockSpec((512, wide), lambda i: (0, i))
    return pl.pallas_call(
        gradient_kernel,
        grid=(BLOCKS,),
        in_specs=[pl.BlockSpec(memory_space=pltpu.SMEM)] + [hbm] * 4 + [block] * len(sent),
        out_specs=block,
        out_shape=jax.ShapeDtypeStruct((512, D), jnp.bfloat16),
        scratch_shapes=[
            pltpu.VMEM((BLOCKS, 2048, wide), jnp.bfloat16),
            pltpu.VMEM((2048, 512), jnp.bfloat16),
            pltpu.VMEM((512, 2048), jnp.bfloat16),
            pltpu.SemaphoreType.DMA((BLOCKS,)),
            pltpu.SemaphoreType.DMA((BLOCKS,)),
        ],
        compiler_params=pltpu.CompilerParams(vmem_limit_bytes=57 << 20),
        name="gradient",
    )(core, *arrays, *sent)


def square_kernel(high, low, direction, out_ref):
    d = direction[...]
    turned = jnp.dot(high[...], d, preferred_element_type=jnp.float32)
    turned = turned + jnp.dot(low[...], d, preferred_element_type=jnp.float32)
    sums = (turned * d.astype(jnp.float32)).reshape(64, 8, 512).sum(axis=0)
    sums = sums[:, :128] + sums[:, 128:256] + sums[:, 256:384] + sums[:, 384:]
    for i in range(8):
        out_ref[i] = sums


def square_sums(high, low, direction):
    vmem = pl.BlockSpec(memory_space=pltpu.VMEM)
    return pl.pallas_call(
        square_kernel,
        in_specs=[vmem] * 3,
        out_specs=vmem,
        out_shape=jax.ShapeDtypeStruct((8, 8, 128), jnp.float32),
        compiler_params=pltpu.CompilerParams(vmem_limit_bytes=8 << 20),
        name="square_sums",
    )(high, low, direction)


CHUNKS = 8


def finish_kernel(
    core_ref,
    at_ref,
    square,
    f0,
    f1,
    d0,
    d1,
    w0,
    w1,
    value_weight,
    output_weight,
    value_copy,
    output_copy,
    value_step,
    value_updated,
    output_step,
    output_updated,
    tiles,
    sems,
):
    rows = D // CHUNKS
    first_core = core_ref[0] == 0

    def scale_of(sums):
        return step_rate / jnp.sqrt(jnp.sum(sums, keepdims=True) / (D * HV) + scale_floor)

    value_scale = scale_of(square[:4].sum(axis=0))
    output_scale = scale_of(square[4:].sum(axis=0))
    scales = (
        jnp.where(first_core, value_scale, output_scale),
        jnp.where(first_core, output_scale, value_scale),
    )

    def sent(out, which, chunk):
        at = pl.ds(chunk * rows, rows)
        return pltpu.make_async_copy(tiles.at[which, at], out.at[at], sems.at[which, chunk])

    for chunk in range(CHUNKS):
        at = pl.ds(chunk * rows, rows)
        for which, (f, d, w) in enumerate(((f0, d0, w0), (f1, d1, w1))):
            whole = jnp.dot(f[at], d[...], preferred_element_type=jnp.float32)
            tile = w[at].astype(jnp.float32) - scales[which] * whole
            tiles[which, at] = tile.astype(jnp.bfloat16)

        @pl.when(first_core)
        def _():
            sent(value_copy, 0, chunk).start()
            sent(output_copy, 1, chunk).start()

        @pl.when(jnp.logical_not(first_core))
        def _():
            sent(output_copy, 0, chunk).start()
            sent(value_copy, 1, chunk).start()

    local = pl.ds(pl.multiple_of(at_ref[0], 64), 64)
    steps = [
        scale * jnp.dot(f[local], d[...], preferred_element_type=jnp.float32)
        for scale, f, d in zip(scales, (f0, f1), (d0, d1))
    ]

    @pl.when(first_core)
    def _():
        value_step[...], output_step[...] = steps

    @pl.when(jnp.logical_not(first_core))
    def _():
        output_step[...], value_step[...] = steps

    value_updated[...] = value_weight[...] - value_step[...]
    output_updated[...] = output_weight[...] - output_step[...]

    for chunk in range(CHUNKS):
        for which in (0, 1):
            sent(value_copy, which, chunk).wait()


def finish(core, at, *arrays):
    smem = pl.BlockSpec(memory_space=pltpu.SMEM)
    vmem = pl.BlockSpec(memory_space=pltpu.VMEM)
    hbm = pl.BlockSpec(memory_space=pltpu.HBM)
    copy = jax.ShapeDtypeStruct((D, 512), jnp.bfloat16)
    local = jax.ShapeDtypeStruct((64, 512), jnp.float32)
    return pl.pallas_call(
        finish_kernel,
        in_specs=[smem] * 2 + [vmem] * 9,
        out_specs=[hbm] * 2 + [vmem] * 4,
        out_shape=[copy] * 2 + [local] * 4,
        scratch_shapes=[
            pltpu.VMEM((2, D, 512), jnp.bfloat16),
            pltpu.SemaphoreType.DMA((2, CHUNKS)),
        ],
        compiler_params=pltpu.CompilerParams(vmem_limit_bytes=12 << 20),
        name="finish",
    )(core, at, *arrays)


def token_sum(rows_in, cols_in):
    return lax.dot_general(
        rows_in, cols_in, (((0,), (0,)), ((), ())), preferred_element_type=jnp.float32
    )


def local(
    model_input,
    value_cotan,
    mixer_cotan,
    head_output,
    value_weight,
    value_factor,
    value_first,
    value_second,
    output_weight,
    output_factor,
    output_first,
    output_second,
):
    core = lax.axis_index(CORE)
    first_core = core == 0

    def pick(a, b):
        return jnp.where(first_core, a, b)

    def chip_rows(mine, theirs):
        return pick(
            jnp.concatenate([mine, theirs], axis=0), jnp.concatenate([theirs, mine], axis=0)
        )

    value_rows = jnp.concatenate([value_factor, value_weight.astype(jnp.bfloat16)], axis=1)
    output_rows = jnp.concatenate([output_factor, output_weight.astype(jnp.bfloat16)], axis=1)
    rows = chip_rows(
        pick(value_rows, output_rows), swapped(pick(output_rows, value_rows))
    )
    group = from_ring(rows, 0)
    group, weight_group = lax.optimization_barrier(
        (jnp.stack([g[:, :512] for g in group]), jnp.stack([g[:, 512:] for g in group]))
    )
    groups = from_ring(group, 1)
    weight_groups = from_ring(weight_group, 1)
    z, y = lax.axis_index("fs_0"), lax.axis_index("fs_1")
    step_b, step_a = jnp.arange(16) // 4, jnp.arange(16) % 4
    index = pick((z + step_b) % 4 * 4 + (y + step_a) % 4, (z + step_a) % 4 * 4 + (y + step_b) % 4)
    index = index.astype(jnp.int32)
    factor = in_chip_order(groups, index).reshape(2048, 512)

    arrays = (model_input, mixer_cotan, value_cotan, head_output)
    grad_theirs = gradient(1 - core.reshape(1), arrays)
    grad_sent = swapped(grad_theirs)
    grad_sum = gradient(core.reshape(1), arrays, (grad_sent,))

    moments_mine = jnp.concatenate(
        [pick(value_first, output_first), pick(value_second, output_second)], axis=1
    )
    moments_theirs = swapped(
        jnp.concatenate(
            [pick(output_first, value_first), pick(output_second, value_second)], axis=1
        )
    )
    moments = chip_rows(moments_mine, moments_theirs)

    part = lax.dot_general(
        factor, grad_sum, (((0,), (1,)), ((), ())), preferred_element_type=jnp.float32
    ).astype(jnp.bfloat16)
    parts = lax.all_to_all(part.reshape(N_ZY, 32, 512), ZY, split_axis=0, concat_axis=0, tiled=True)
    projected = parts.astype(jnp.float32).sum(axis=0)
    first_new = beta_first * moments[:, :512] + (1.0 - beta_first) * projected
    second_new = beta_second * moments[:, 512:] + (1.0 - beta_second) * projected * projected
    direction = (first_new / (jnp.sqrt(second_new) + tiny_eps)).astype(jnp.bfloat16)
    direction = sent_to_chips(direction)

    gram = token_sum(factor, factor)
    gram_high = lax.optimization_barrier(gram.astype(jnp.bfloat16))
    gram_low = (gram - gram_high.astype(jnp.float32)).astype(jnp.bfloat16)
    gram_low = lax.optimization_barrier(gram_low)
    square = square_sums(gram_high, gram_low, direction)
    square = lax.all_to_all(square, (CORE, "tp"), split_axis=0, concat_axis=0, tiled=True)
    factor_other = swapped(factor)
    weight = in_chip_order(weight_groups, index).reshape(2048, 512)
    weight_other = swapped(weight)
    direction_other = swapped(direction)
    value_copy, output_copy, value_step, value_updated, output_step, output_updated = finish(
        core.reshape(1),
        (lax.axis_index(FS) * 64).reshape(1),
        square,
        factor,
        factor_other,
        direction,
        direction_other,
        weight,
        weight_other,
        value_weight,
        output_weight,
    )

    news = jnp.concatenate([first_new, second_new], axis=1)
    upper, lower = news[:16], news[16:]
    news_mine = pick(upper, lower)
    news_theirs = swapped(pick(lower, upper))
    value_news, output_news = pick(news_mine, news_theirs), pick(news_theirs, news_mine)
    value_fnew, value_snew = value_news[:, :512], value_news[:, 512:]
    output_fnew, output_snew = output_news[:, :512], output_news[:, 512:]
    return (
        value_step,
        value_updated,
        value_fnew,
        value_snew,
        value_copy,
        output_step,
        output_updated,
        output_fnew,
        output_snew,
        output_copy,
    )


def solution(mesh):
    torus = Mesh(mesh.devices.reshape(4, 4, 2, mesh.shape["tp"]), ("fs_0", "fs_1", "fs_2", "tp"))
    in_specs = (
        P(FS, None),
        P(FS, "tp"),
        P(FS, None),
        P(FS, "tp"),
        P(FS, "tp"),
        P(FS, None),
        P(FS, "tp"),
        P(FS, "tp"),
        P(FS, "tp"),
        P(FS, None),
        P(FS, "tp"),
        P(FS, "tp"),
    )
    out_specs = (
        P(FS, "tp"),
        P(FS, "tp"),
        P(FS, "tp"),
        P(FS, "tp"),
        P(None, "tp"),
        P(FS, "tp"),
        P(FS, "tp"),
        P(FS, "tp"),
        P(FS, "tp"),
        P(None, "tp"),
    )

    return jax.shard_map(local, mesh=torus, in_specs=in_specs, out_specs=out_specs, check_vma=False)
```

```python
import jax
import jax.numpy as jnp
from jax import lax
from jax.sharding import Mesh
from jax.sharding import PartitionSpec as P
from jax.experimental import pallas as pl
from jax.experimental.pallas import tpu as pltpu

D = 2048
HV = 2048
ZY = ("fs_0", "fs_1")
CORE = "fs_2"
FS = ("fs_0", "fs_1", "fs_2")
N_ZY = 16

beta_first = 0.8
beta_second = 0.9
step_rate = 0.02
scale_floor = 0.25
tiny_eps = 1e-08

SWAP = [(0, 1), (1, 0)]


def swapped(x):
    return lax.ppermute(x, CORE, SWAP)


def sent_to_chips(x):
    copies = jnp.broadcast_to(x, (N_ZY, *x.shape))
    parts = lax.all_to_all(copies, ZY, split_axis=0, concat_axis=0, tiled=True)
    return parts.reshape(N_ZY * x.shape[0], x.shape[1])


def place(z, y, core):
    return (z % 4 * 4 + y % 4) * 2 + core


def ring_pairs(shift, along_y_core):
    pairs = []
    for z in range(4):
        for y in range(4):
            for core in range(2):
                to = (z, y - shift) if core == along_y_core else (z - shift, y)
                pairs.append((place(z, y, core), place(*to, core)))
    return pairs


def from_ring(x, along_y_core):
    received = []
    for shift in (1, 2, 3):
        received.append(lax.ppermute(x, FS, ring_pairs(shift, along_y_core)))
    return [x] + received


def order_kernel(index_ref, *refs):
    out_ref = refs[-1]
    for b in range(4):
        for a in range(4):
            out_ref[index_ref[b * 4 + a]] = refs[b][a]


def in_chip_order(groups, index):
    vmem = pl.BlockSpec(memory_space=pltpu.VMEM)
    return pl.pallas_call(
        order_kernel,
        in_specs=[pl.BlockSpec(memory_space=pltpu.SMEM)] + [vmem] * 4,
        out_specs=vmem,
        out_shape=jax.ShapeDtypeStruct((N_ZY, 128, 512), jnp.bfloat16),
        compiler_params=pltpu.CompilerParams(vmem_limit_bytes=8 << 20),
        name="in_chip_order",
    )(index, *groups)


BLOCKS = 2


def gradient_kernel(core_ref, *refs):
    rows, cols = refs[:2], refs[2:4]
    sent = refs[4:-6]
    out_ref, rows_buf, cols_buf, turned, rows_sems, cols_sems = refs[-6:]
    step = pl.program_id(0)
    wide = D // BLOCKS

    def rows_copy(which, block):
        at = pl.ds(block * wide, wide)
        return pltpu.make_async_copy(
            rows[which].at[:, at], rows_buf.at[block], rows_sems.at[block]
        )

    def cols_copy(which, block):
        at = pl.ds(block * wide, wide)
        return pltpu.make_async_copy(cols[which].at[at], cols_buf.at[at], cols_sems.at[block])

    @pl.when(step == 0)
    def _():
        for which in (0, 1):

            @pl.when(core_ref[0] == which)
            def _():
                for block in range(BLOCKS):
                    cols_copy(which, block).start()
                for block in range(BLOCKS):
                    rows_copy(which, block).start()

        for block in range(BLOCKS):
            cols_copy(0, block).wait()
            at = pl.ds(block * wide, wide)
            turned[:, at] = cols_buf[at].T

    rows_copy(0, step).wait()
    grad = jnp.dot(turned[...], rows_buf[step], preferred_element_type=jnp.float32)
    for ref in sent:
        grad = grad + ref[...].astype(jnp.float32)
    out_ref[...] = grad.astype(jnp.bfloat16)


def gradient(core, arrays, sent=()):
    hbm = pl.BlockSpec(memory_space=pltpu.HBM)
    wide = D // BLOCKS
    block = pl.BlockSpec((512, wide), lambda i: (0, i))
    return pl.pallas_call(
        gradient_kernel,
        grid=(BLOCKS,),
        in_specs=[pl.BlockSpec(memory_space=pltpu.SMEM)] + [hbm] * 4 + [block] * len(sent),
        out_specs=block,
        out_shape=jax.ShapeDtypeStruct((512, D), jnp.bfloat16),
        scratch_shapes=[
            pltpu.VMEM((BLOCKS, 2048, wide), jnp.bfloat16),
            pltpu.VMEM((2048, 512), jnp.bfloat16),
            pltpu.VMEM((512, 2048), jnp.bfloat16),
            pltpu.SemaphoreType.DMA((BLOCKS,)),
            pltpu.SemaphoreType.DMA((BLOCKS,)),
        ],
        compiler_params=pltpu.CompilerParams(vmem_limit_bytes=57 << 20),
        name="gradient",
    )(core, *arrays, *sent)


def square_kernel(high, low, direction, out_ref):
    d = direction[...]
    turned = jnp.dot(high[...], d, preferred_element_type=jnp.float32)
    turned = turned + jnp.dot(low[...], d, preferred_element_type=jnp.float32)
    sums = (turned * d.astype(jnp.float32)).reshape(64, 8, 512).sum(axis=0)
    sums = sums[:, :128] + sums[:, 128:256] + sums[:, 256:384] + sums[:, 384:]
    for i in range(8):
        out_ref[i] = sums


def square_sums(high, low, direction):
    vmem = pl.BlockSpec(memory_space=pltpu.VMEM)
    return pl.pallas_call(
        square_kernel,
        in_specs=[vmem] * 3,
        out_specs=vmem,
        out_shape=jax.ShapeDtypeStruct((8, 8, 128), jnp.float32),
        compiler_params=pltpu.CompilerParams(vmem_limit_bytes=8 << 20),
        name="square_sums",
    )(high, low, direction)


CHUNKS = 8


def finish_kernel(
    core_ref,
    at_ref,
    square,
    f0,
    f1,
    d0,
    d1,
    w0,
    w1,
    value_weight,
    output_weight,
    value_copy,
    output_copy,
    value_step,
    value_updated,
    output_step,
    output_updated,
    tiles,
    sems,
    locals_new,
    local_sems,
):
    rows = D // CHUNKS
    first_core = core_ref[0] == 0

    def scale_of(sums):
        return step_rate / jnp.sqrt(jnp.sum(sums, keepdims=True) / (D * HV) + scale_floor)

    value_scale = scale_of(square[:4].sum(axis=0))
    output_scale = scale_of(square[4:].sum(axis=0))
    scales = (
        jnp.where(first_core, value_scale, output_scale),
        jnp.where(first_core, output_scale, value_scale),
    )

    def sent(out, which, chunk):
        at = pl.ds(chunk * rows, rows)
        return pltpu.make_async_copy(tiles.at[which, at], out.at[at], sems.at[which, chunk])

    local = pl.ds(pl.multiple_of(at_ref[0], 64), 64)
    steps = [
        scale * jnp.dot(f[local], d[...], preferred_element_type=jnp.float32)
        for scale, f, d in zip(scales, (f0, f1), (d0, d1))
    ]
    value_new = jnp.where(first_core, steps[0], steps[1])
    output_new = jnp.where(first_core, steps[1], steps[0])
    locals_new[0] = value_new
    locals_new[1] = value_weight[...] - value_new
    locals_new[2] = output_new
    locals_new[3] = output_weight[...] - output_new
    local_copies = [
        pltpu.make_async_copy(locals_new.at[i], out, local_sems.at[i])
        for i, out in enumerate((value_step, value_updated, output_step, output_updated))
    ]
    for copy in local_copies:
        copy.start()

    for chunk in range(CHUNKS):
        at = pl.ds(chunk * rows, rows)
        for which, (f, d, w) in enumerate(((f0, d0, w0), (f1, d1, w1))):
            whole = jnp.dot(f[at], d[...], preferred_element_type=jnp.float32)
            tile = w[at].astype(jnp.float32) - scales[which] * whole
            tiles[which, at] = tile.astype(jnp.bfloat16)

        @pl.when(first_core)
        def _():
            sent(value_copy, 0, chunk).start()
            sent(output_copy, 1, chunk).start()

        @pl.when(jnp.logical_not(first_core))
        def _():
            sent(output_copy, 0, chunk).start()
            sent(value_copy, 1, chunk).start()

    for chunk in range(CHUNKS):
        for which in (0, 1):
            sent(value_copy, which, chunk).wait()
    for copy in local_copies:
        copy.wait()


def finish(core, at, *arrays):
    smem = pl.BlockSpec(memory_space=pltpu.SMEM)
    vmem = pl.BlockSpec(memory_space=pltpu.VMEM)
    hbm = pl.BlockSpec(memory_space=pltpu.HBM)
    copy = jax.ShapeDtypeStruct((D, 512), jnp.bfloat16)
    local = jax.ShapeDtypeStruct((64, 512), jnp.float32)
    return pl.pallas_call(
        finish_kernel,
        in_specs=[smem] * 2 + [vmem] * 9,
        out_specs=[hbm] * 6,
        out_shape=[copy] * 2 + [local] * 4,
        scratch_shapes=[
            pltpu.VMEM((2, D, 512), jnp.bfloat16),
            pltpu.SemaphoreType.DMA((2, CHUNKS)),
            pltpu.VMEM((4, 64, 512), jnp.float32),
            pltpu.SemaphoreType.DMA((4,)),
        ],
        compiler_params=pltpu.CompilerParams(vmem_limit_bytes=12 << 20),
        name="finish",
    )(core, at, *arrays)


def token_sum(rows_in, cols_in):
    return lax.dot_general(
        rows_in, cols_in, (((0,), (0,)), ((), ())), preferred_element_type=jnp.float32
    )


def local(
    model_input,
    value_cotan,
    mixer_cotan,
    head_output,
    value_weight,
    value_factor,
    value_first,
    value_second,
    output_weight,
    output_factor,
    output_first,
    output_second,
):
    core = lax.axis_index(CORE)
    first_core = core == 0

    def pick(a, b):
        return jnp.where(first_core, a, b)

    def chip_rows(mine, theirs):
        return pick(
            jnp.concatenate([mine, theirs], axis=0), jnp.concatenate([theirs, mine], axis=0)
        )

    value_rows = jnp.concatenate([value_factor, value_weight.astype(jnp.bfloat16)], axis=1)
    output_rows = jnp.concatenate([output_factor, output_weight.astype(jnp.bfloat16)], axis=1)
    rows = chip_rows(
        pick(value_rows, output_rows), swapped(pick(output_rows, value_rows))
    )
    group = from_ring(rows, 0)
    group, weight_group = lax.optimization_barrier(
        (jnp.stack([g[:, :512] for g in group]), jnp.stack([g[:, 512:] for g in group]))
    )
    groups = from_ring(group, 1)
    weight_groups = from_ring(weight_group, 1)
    z, y = lax.axis_index("fs_0"), lax.axis_index("fs_1")
    step_b, step_a = jnp.arange(16) // 4, jnp.arange(16) % 4
    index = pick((z + step_b) % 4 * 4 + (y + step_a) % 4, (z + step_a) % 4 * 4 + (y + step_b) % 4)
    index = index.astype(jnp.int32)
    factor = in_chip_order(groups, index).reshape(2048, 512)

    arrays = (model_input, mixer_cotan, value_cotan, head_output)
    grad_theirs = gradient(1 - core.reshape(1), arrays)
    grad_sent = swapped(grad_theirs)
    grad_sum = gradient(core.reshape(1), arrays, (grad_sent,))

    moments_mine = jnp.concatenate(
        [pick(value_first, output_first), pick(value_second, output_second)], axis=1
    )
    moments_theirs = swapped(
        jnp.concatenate(
            [pick(output_first, value_first), pick(output_second, value_second)], axis=1
        )
    )
    moments = chip_rows(moments_mine, moments_theirs)

    part = lax.dot_general(
        factor, grad_sum, (((0,), (1,)), ((), ())), preferred_element_type=jnp.float32
    ).astype(jnp.bfloat16)
    parts = lax.all_to_all(part.reshape(N_ZY, 32, 512), ZY, split_axis=0, concat_axis=0, tiled=True)
    projected = parts.astype(jnp.float32).sum(axis=0)
    first_new = beta_first * moments[:, :512] + (1.0 - beta_first) * projected
    second_new = beta_second * moments[:, 512:] + (1.0 - beta_second) * projected * projected
    direction = (first_new / (jnp.sqrt(second_new) + tiny_eps)).astype(jnp.bfloat16)
    direction = sent_to_chips(direction)

    gram = token_sum(factor, factor)
    gram_high = lax.optimization_barrier(gram.astype(jnp.bfloat16))
    gram_low = (gram - gram_high.astype(jnp.float32)).astype(jnp.bfloat16)
    gram_low = lax.optimization_barrier(gram_low)
    square = square_sums(gram_high, gram_low, direction)
    square = lax.all_to_all(square, (CORE, "tp"), split_axis=0, concat_axis=0, tiled=True)
    factor_other = swapped(factor)
    weight = in_chip_order(weight_groups, index).reshape(2048, 512)
    weight_other = swapped(weight)
    direction_other = swapped(direction)
    value_copy, output_copy, value_step, value_updated, output_step, output_updated = finish(
        core.reshape(1),
        (lax.axis_index(FS) * 64).reshape(1),
        square,
        factor,
        factor_other,
        direction,
        direction_other,
        weight,
        weight_other,
        value_weight,
        output_weight,
    )

    news = jnp.concatenate([first_new, second_new], axis=1)
    upper, lower = news[:16], news[16:]
    news_mine = pick(upper, lower)
    news_theirs = swapped(pick(lower, upper))
    value_news, output_news = pick(news_mine, news_theirs), pick(news_theirs, news_mine)
    value_fnew, value_snew = value_news[:, :512], value_news[:, 512:]
    output_fnew, output_snew = output_news[:, :512], output_news[:, 512:]
    return (
        value_step,
        value_updated,
        value_fnew,
        value_snew,
        value_copy,
        output_step,
        output_updated,
        output_fnew,
        output_snew,
        output_copy,
    )


def solution(mesh):
    torus = Mesh(mesh.devices.reshape(4, 4, 2, mesh.shape["tp"]), ("fs_0", "fs_1", "fs_2", "tp"))
    in_specs = (
        P(FS, None),
        P(FS, "tp"),
        P(FS, None),
        P(FS, "tp"),
        P(FS, "tp"),
        P(FS, None),
        P(FS, "tp"),
        P(FS, "tp"),
        P(FS, "tp"),
        P(FS, None),
        P(FS, "tp"),
        P(FS, "tp"),
    )
    out_specs = (
        P(FS, "tp"),
        P(FS, "tp"),
        P(FS, "tp"),
        P(FS, "tp"),
        P(None, "tp"),
        P(FS, "tp"),
        P(FS, "tp"),
        P(FS, "tp"),
        P(FS, "tp"),
        P(None, "tp"),
    )

    return jax.shard_map(local, mesh=torus, in_specs=in_specs, out_specs=out_specs, check_vma=False)
```
